256 devices in a mesh: sp: 16 (over y, x), dp: 16 (over z, core).
Axes of the slice: x: 4, y: 4, z: 8, core: 2. Of those that a mesh axis runs over, the one named last changes fastest.
Arguments:
- tokens: bfloat16 [16, 5120, 2048], P('dp', 'sp'), may hold values from -6 to 6
- up_weight: bfloat16 [2048, 2048], P('dp'), may hold values from -0.125 to 0.125
- gate_weight: bfloat16 [2048, 2048], P('dp'), may hold values from -0.125 to 0.125
- group_gain: float32 [16, 128], P('sp'), may hold values from 0.1 to 1.9
- mix_weight: bfloat16 [16, 1280, 1280], P('sp', 'dp'), may hold values from -0.15625 to 0.15625
- mix_bias: float32 [16, 1280], P('sp'), may hold values from 0.5 to 1.5
- out_gain: float32 [2048], replicated, may hold values from 0.1 to 1.9
- out_weight: bfloat16 [2048, 2048], P(None, 'dp'), may hold values from -0.125 to 0.125
Outputs:
- mixed_out: bfloat16 [16, 5120, 2048], P('dp', 'sp')
The draws below stay inside these ranges and needn't reach their ends.
All inputs are finite; a program needn't handle non-finite values.
Results may differ from the reference program's by a relative error of at most 0.0072.
Values may be sent and summed in bfloat16 or wider, within the bound.
No kernel may reach another device: no remote copies, remote signals or barrier semaphores. Data moves between devices by JAX's collectives and lax.ppermute only.
A program may use at most 128 MiB of HBM per device.

```python
import jax
import jax.numpy as jnp
from jax import lax

D = 2048
GROUPS = 16
GROUP_DIM = 128
SPAN = 1280
WIDTH = 2048
LENGTH = 5120
SEQS = 16


def level_of(key, extent, cuts, smallest, top_value):
    level, own = 1.0, jax.random.fold_in(key, 6)
    for axis_at, parts in cuts:
        steps = jnp.exp(jax.random.uniform(jax.random.fold_in(own, axis_at), (parts,), jnp.float32, smallest / len(cuts), top_value / len(cuts)))
        level = level * jnp.repeat(steps, extent[axis_at] // parts).reshape([-1 if axis == axis_at else 1 for axis in range(len(extent))])
    return level


def normal_values(own_key, dims, deviation, most, cuts=(), held_as=jnp.bfloat16):
    entries = deviation * jax.random.normal(own_key, dims, jnp.float32)
    if cuts:
        entries = entries * level_of(own_key, dims, cuts, -0.22, 0.18)
    return jnp.clip(entries, -most, most).astype(held_as)


def setup_inputs(seed: int = 0) -> dict:
    splits = jax.random.split(jax.random.key(seed), 9)
    tokens = normal_values(splits[0], (SEQS, LENGTH, D), 1.0, 6.0, ((0, 16), (1, 16)))
    up_weight = normal_values(splits[1], (D, WIDTH), D ** -0.5, 0.125, ((0, 16),))
    gate_weight = normal_values(splits[2], (D, WIDTH), D ** -0.5, 0.125, ((0, 16),))
    group_gain = jnp.clip(1.0 + 0.18 * jax.random.normal(splits[3], (GROUPS, GROUP_DIM), jnp.float32), 0.1, 1.9)
    mix_weight = normal_values(splits[4], (GROUPS, SPAN, SPAN), SPAN ** -0.5, 0.15625, ((0, 16), (1, 16)))
    mix_bias = jnp.clip(0.5 + 1.0 * jax.random.uniform(splits[5], (GROUPS, SPAN), jnp.float32) ** level_of(splits[5], (GROUPS, SPAN), ((0, 16),), -0.2, 0.2), 0.5, 1.5)
    out_gain = jnp.clip(1.0 + 0.18 * jax.random.normal(splits[6], (WIDTH,), jnp.float32), 0.1, 1.9)
    out_weight = normal_values(splits[7], (WIDTH, D), WIDTH ** -0.5, 0.125, ((1, 16),))
    return {"tokens": tokens, "up_weight": up_weight, "gate_weight": gate_weight, "group_gain": group_gain, "mix_weight": mix_weight, "mix_bias": mix_bias, "out_gain": out_gain, "out_weight": out_weight}


norm_eps = 1e-06

def reference(tokens, up_weight, gate_weight, group_gain, mix_weight, mix_bias, out_gain, out_weight):
    lower = jnp.tril(jnp.ones((SPAN, SPAN), dtype=bool))
    mix_mask = jnp.where(lower[None], mix_weight, jnp.zeros_like(mix_weight)).astype(jnp.float32)
    bias_cols = mix_bias.astype(jnp.float32).T

    def one_sequence(sequence):
        up_proj = jnp.dot(sequence, up_weight, preferred_element_type=jnp.float32).astype(jnp.bfloat16)
        gate_proj = jnp.dot(sequence, gate_weight, preferred_element_type=jnp.float32).astype(jnp.bfloat16)
        up_proj = lax.optimization_barrier(up_proj)
        gate_proj = lax.optimization_barrier(gate_proj)
        opened = jax.nn.gelu(up_proj.astype(jnp.float32)).reshape(LENGTH, GROUPS, GROUP_DIM)
        gate_act = jax.nn.gelu(gate_proj.astype(jnp.float32)).reshape(LENGTH, GROUPS, GROUP_DIM)
        center = lax.optimization_barrier(jnp.mean(gate_act, axis=-1, keepdims=True))
        spread = lax.optimization_barrier(jnp.mean(jnp.square(gate_act - center), axis=-1, keepdims=True))
        normal_v = ((gate_act - center) * lax.rsqrt(spread + norm_eps) * group_gain.astype(jnp.float32)).astype(jnp.bfloat16)
        normal_v = lax.optimization_barrier(normal_v)
        blocks = normal_v.astype(jnp.float32).reshape(LENGTH // SPAN, SPAN, GROUPS, GROUP_DIM)
        mixed_sum = jnp.einsum('gij,njgc->nigc', mix_mask, blocks) + bias_cols[None, :, :, None]
        gated = (opened * mixed_sum.reshape(LENGTH, GROUPS, GROUP_DIM)).astype(jnp.bfloat16)
        gated = lax.optimization_barrier(gated)
        gated_f = gated.astype(jnp.float32).reshape(LENGTH, WIDTH)
        scale = lax.rsqrt(lax.optimization_barrier(jnp.mean(gated_f * gated_f, axis=-1, keepdims=True)) + norm_eps)
        normed = (gated_f * scale * out_gain.astype(jnp.float32)).astype(jnp.bfloat16)
        return jnp.dot(normed, out_weight, preferred_element_type=jnp.float32).astype(jnp.bfloat16)
    return lax.map(one_sequence, tokens)
```

```python
import functools

import jax
import jax.numpy as jnp
from jax import lax
from jax.experimental import pallas as pl
from jax.experimental.pallas import tpu as pltpu
from jax.sharding import PartitionSpec as P


norm_eps = 1e-06
bf16 = jnp.bfloat16
f32 = jnp.float32

ROW = 4
DP = 16
C = 128
POS = 320
HALF = POS // 2
SPAN = 1280
D = 2048
K_DEV = D // DP
M_DEV = SPAN // DP
PROJ = ROW * K_DEV
MIXR = (SPAN // C) * M_DEV
PACK = 2 * PROJ + MIXR
VMEM_LIMIT = 60 * 1024 * 1024

along_x = [(y * 4 + x, y * 4 + (x + 1) % 4) for y in range(4) for x in range(4)]
against_x = [(b, a) for a, b in along_x]
rows_of_x = [[y * 4 + x for x in range(4)] for y in range(4)]
cols_of_y = [[y * 4 + x for y in range(4)] for x in range(4)]

vmem = pl.BlockSpec(memory_space=pltpu.VMEM)
hbm = pl.BlockSpec(memory_space=pl.ANY)
smem = pl.BlockSpec(memory_space=pltpu.SMEM)


def params():
    return pltpu.CompilerParams(vmem_limit_bytes=VMEM_LIMIT)


def pack_kernel(x_ref, gate_ref, up_ref, mix_ref, out_ref):
    x = x_ref[0]
    for k in range(ROW):
        col = pl.multiple_of((ROW * k + x) * C, C)
        out_ref[k * K_DEV : (k + 1) * K_DEV, :] = gate_ref[:, pl.ds(col, C)]
        out_ref[PROJ + k * K_DEV : PROJ + (k + 1) * K_DEV, :] = up_ref[:, pl.ds(col, C)]
    for k in range(SPAN // C):
        out_ref[2 * PROJ + k * M_DEV : 2 * PROJ + (k + 1) * M_DEV, :] = mix_ref[:, k * C : (k + 1) * C]


def gelu(v):
    return jax.nn.gelu(v, approximate=True)


def project_kernel(first, gated, x_ref, packed_ref, *refs):
    tokens, (out_ref, w_ref, sems) = refs[:7], refs[7:]
    copies = []
    for k in range(ROW):
        copies.append(
            pltpu.make_async_copy(
                packed_ref.at[:, first + k * K_DEV : first + (k + 1) * K_DEV, :],
                w_ref.at[:, :, k * C : (k + 1) * C],
                sems.at[k],
            )
        )
    for copy in copies:
        copy.start()
    for copy in copies:
        copy.wait()
    weight = w_ref[...].reshape(D, ROW * C)
    x = x_ref[0]
    own, left_a, left_b, right_a, right_b, far_a, far_b = tokens
    pieces = (
        (own, 0, 0, 0),
        (own, HALF, 0, HALF),
        (left_a, 0, 3, 0),
        (left_b, 0, 3, HALF),
        (right_a, 0, 1, 0),
        (right_b, 0, 1, HALF),
        (far_a, 0, 2, 0),
        (far_b, 0, 2, HALF),
    )
    for ref, begin, shift, offset in pieces:
        made = jnp.dot(ref[begin : begin + HALF, :], weight, preferred_element_type=f32).astype(bf16)
        row = pl.multiple_of(lax.rem(x + shift, ROW) * POS + offset, HALF)
        if not gated:
            out_ref[pl.ds(row, HALF), :] = made
            continue
        act = gelu(made.astype(f32))
        for k in range(ROW):
            part = act[:, k * C : (k + 1) * C]
            center = jnp.mean(part, axis=-1, keepdims=True)
            part = part - center
            spread = jnp.mean(part * part, axis=-1, keepdims=True)
            out_ref[k, pl.ds(row, HALF), :] = (part * lax.rsqrt(spread + norm_eps)).astype(bf16)


def project(x, packed, tokens, gated):
    shape = (ROW, SPAN, C) if gated else (SPAN, ROW * C)
    return pl.pallas_call(
        functools.partial(project_kernel, 0 if gated else PROJ, gated),
        out_shape=jax.ShapeDtypeStruct(shape, bf16),
        in_specs=[smem, hbm] + [vmem] * 7,
        out_specs=vmem,
        scratch_shapes=[pltpu.VMEM((DP, K_DEV, ROW * C), bf16), pltpu.SemaphoreType.DMA((ROW,))],
        compiler_params=params(),
        cost_estimate=pl.CostEstimate(
            flops=2 * SPAN * D * ROW * C, bytes_accessed=10_000_000, transcendentals=SPAN * ROW * C
        ),
        name="gate_rows" if gated else "up_rows",
    )(x, packed, *tokens)


def mix_kernel(packed_ref, nv_ref, gain_ref, bias_ref, out_ref, m_ref, sems):
    copies = []
    for k in range(SPAN // C):
        begin = 2 * PROJ + k * M_DEV
        copies.append(
            pltpu.make_async_copy(
                packed_ref.at[:, begin : begin + M_DEV, :], m_ref.at[:, :, k * C : (k + 1) * C], sems.at[k]
            )
        )
    for copy in copies:
        copy.start()
    bias = jnp.broadcast_to(bias_ref[...], (C, SPAN)).T
    gain = gain_ref[...]
    for copy in copies:
        copy.wait()
    values = jnp.concatenate([nv_ref[n] for n in range(ROW)], axis=1)
    per = POS // M_DEV
    for t in range(ROW):
        width = -(-(t + 1) * POS // C) * C
        rows = m_ref[t * per : (t + 1) * per, :, :width].reshape(POS, width)
        i = lax.broadcasted_iota(jnp.int32, (POS, width), 0) + t * POS
        j = lax.broadcasted_iota(jnp.int32, (POS, width), 1)
        rows = jnp.where(j <= i, rows, jnp.zeros_like(rows))
        made = jnp.dot(rows, values[:width, :], preferred_element_type=f32)
        for n in range(ROW):
            part = made[:, n * C : (n + 1) * C] * gain + bias[t * POS : (t + 1) * POS, :]
            out_ref[n * ROW + t] = part.astype(bf16)


def mix(packed, nv, gain, bias):
    return pl.pallas_call(
        mix_kernel,
        out_shape=jax.ShapeDtypeStruct((ROW * ROW, POS, C), bf16),
        in_specs=[hbm, vmem, vmem, vmem],
        out_specs=vmem,
        scratch_shapes=[pltpu.VMEM((DP, M_DEV, SPAN), bf16), pltpu.SemaphoreType.DMA((SPAN // C,))],
        compiler_params=params(),
        cost_estimate=pl.CostEstimate(flops=2 * SPAN * SPAN * ROW * C, bytes_accessed=7_000_000, transcendentals=0),
        name="mix_positions",
    )(packed, nv, gain, bias)


def out_kernel(mixed_ref, up_ref, gain_ref, w_ref, out_ref, normed_ref):
    @pl.when(pl.program_id(0) == 0)
    def _():
        total = jnp.zeros((POS, C), f32)
        for g in range(ROW * ROW):
            y, x = divmod(g, ROW)
            opened = gelu(up_ref[x, :, y * C : (y + 1) * C].astype(f32))
            gated = (opened * mixed_ref[g].astype(f32)).astype(bf16)
            normed_ref[:, g * C : (g + 1) * C] = gated
            gated = gated.astype(f32)
            total = total + gated * gated
        scale = lax.rsqrt(jnp.sum(total, axis=-1, keepdims=True) / D + norm_eps)
        for g in range(ROW * ROW):
            cols = slice(g * C, (g + 1) * C)
            normed_ref[:, cols] = (normed_ref[:, cols].astype(f32) * scale * gain_ref[:, cols]).astype(bf16)

    weight = jnp.concatenate([w_ref[0], w_ref[1]], axis=1)
    out_ref[...] = jnp.dot(normed_ref[...], weight, preferred_element_type=f32).astype(bf16)


def out_project(mixed, up, gain, weights):
    return pl.pallas_call(
        out_kernel,
        grid=(DP // 2,),
        out_shape=jax.ShapeDtypeStruct((POS, D), bf16),
        in_specs=[
            pl.BlockSpec((ROW * ROW, POS, C), lambda n: (0, 0, 0)),
            pl.BlockSpec((ROW, POS, ROW * C), lambda n: (0, 0, 0)),
            pl.BlockSpec((1, D), lambda n: (0, 0)),
            pl.BlockSpec((2, D, K_DEV), lambda n: (n, 0, 0)),
        ],
        out_specs=pl.BlockSpec((POS, 2 * K_DEV), lambda n: (0, n)),
        scratch_shapes=[pltpu.VMEM((POS, D), bf16)],
        compiler_params=params(),
        cost_estimate=pl.CostEstimate(flops=2 * POS * D * D, bytes_accessed=13_000_000, transcendentals=POS * D),
        name="norm_out",
    )(mixed, up, gain, weights)


def body(tokens, up_weight, gate_weight, group_gain, mix_weight, mix_bias, out_gain, out_weight):
    own = tokens[0]
    x = lax.rem(lax.axis_index("sp"), ROW).astype(jnp.int32).reshape(1)
    packed_own = pl.pallas_call(
        pack_kernel,
        out_shape=jax.ShapeDtypeStruct((PACK, C), bf16),
        in_specs=[smem, vmem, vmem, vmem],
        out_specs=vmem,
        compiler_params=params(),
        name="pack_rows",
    )(x, gate_weight, up_weight, mix_weight[0])
    packed = lax.all_gather(packed_own, "dp")
    out_shard, _ = lax.optimization_barrier((out_weight, packed_own))
    out_blocks = lax.all_gather(out_shard, "dp")

    head, tail = own[:HALF], own[HALF:]
    left_a = lax.ppermute(head, "sp", along_x)
    right_b = lax.ppermute(tail, "sp", against_x)
    left_b = lax.ppermute(tail, "sp", along_x)
    right_a = lax.ppermute(head, "sp", against_x)
    far_a = lax.ppermute(left_a, "sp", along_x)
    far_b = lax.ppermute(right_b, "sp", against_x)
    rows = (own, left_a, left_b, right_a, right_b, far_a, far_b)

    nv = project(x, packed, rows, True)
    nv = lax.all_to_all(nv, "sp", split_axis=0, concat_axis=0, tiled=True, axis_index_groups=cols_of_y)
    up = project(x, packed, rows, False).reshape(ROW, POS, ROW * C)
    up = lax.all_to_all(up, "sp", split_axis=0, concat_axis=0, tiled=True, axis_index_groups=rows_of_x)
    mixed = mix(packed, nv, group_gain, mix_bias)
    mixed = lax.all_to_all(mixed, "sp", split_axis=0, concat_axis=0, tiled=True)
    return out_project(mixed, up, out_gain.reshape(1, D), out_blocks)[None]


def solution(mesh):
    return jax.shard_map(
        body,
        mesh=mesh,
        in_specs=(
            P("dp", "sp", None),
            P("dp", None),
            P("dp", None),
            P("sp", None),
            P("sp", "dp", None),
            P("sp", None),
            P(),
            P(None, "dp"),
        ),
        out_specs=P("dp", "sp", None),
        check_vma=False,
    )
```

```python
import jax
import jax.numpy as jnp
from jax import lax
from jax.experimental import pallas as pl
from jax.experimental.pallas import tpu as pltpu
from jax.sharding import PartitionSpec as P


norm_eps = 1e-06
bf16 = jnp.bfloat16
f32 = jnp.float32

ROW = 4
DP = 16
C = 128
POS = 320
HALF = POS // 2
SPAN = 1280
D = 2048
K_DEV = D // DP
M_DEV = SPAN // DP
PROJ = ROW * K_DEV
MIXR = (SPAN // C) * M_DEV
PACK = 2 * PROJ + MIXR

along_x = [(y * 4 + x, y * 4 + (x + 1) % 4) for y in range(4) for x in range(4)]
against_x = [(b, a) for a, b in along_x]
across_x = [(y * 4 + x, y * 4 + (x + 2) % 4) for y in range(4) for x in range(4)]
along_y = [(y * 4 + x, (y + 1) % 4 * 4 + x) for y in range(4) for x in range(4)]
against_y = [(b, a) for a, b in along_y]
across_y = [(y * 4 + x, (y + 2) % 4 * 4 + x) for y in range(4) for x in range(4)]

vmem = pl.BlockSpec(memory_space=pltpu.VMEM)
hbm = pl.BlockSpec(memory_space=pltpu.HBM)
smem = pl.BlockSpec(memory_space=pltpu.SMEM)


def params(mib):
    return pltpu.CompilerParams(vmem_limit_bytes=mib * 1024 * 1024)


def pack_kernel(at_ref, gate_ref, up_ref, mix_ref, out_ref, sems):
    x = at_ref[1]
    copies = []
    for k in range(ROW):
        col = pl.multiple_of((ROW * k + x) * C, C)
        copies.append((gate_ref.at[:, pl.ds(col, C)], out_ref.at[k * K_DEV : (k + 1) * K_DEV, :]))
        copies.append((up_ref.at[:, pl.ds(col, C)], out_ref.at[PROJ + k * K_DEV : PROJ + (k + 1) * K_DEV, :]))
    for k in range(SPAN // C):
        begin = 2 * PROJ + k * M_DEV
        copies.append((mix_ref.at[:, k * C : (k + 1) * C], out_ref.at[begin : begin + M_DEV, :]))
    copies = [pltpu.make_async_copy(a, b, sems.at[n]) for n, (a, b) in enumerate(copies)]
    for copy in copies:
        copy.start()
    for copy in copies:
        copy.wait()


def gelu(v):
    return jax.nn.gelu(v, approximate=True)


def gate_kernel(at_ref, packed_ref, *refs):
    tokens, outs, (w_ref, sems) = refs[:7], refs[7:11], refs[11:]
    y = at_ref[0]
    x = at_ref[1]
    copies = []
    for d in range(ROW):
        begin = pl.multiple_of(lax.rem(y + d, ROW) * K_DEV, K_DEV)
        copies.append(
            pltpu.make_async_copy(
                packed_ref.at[:, pl.ds(begin, K_DEV), :], w_ref.at[:, :, d * C : (d + 1) * C], sems.at[d]
            )
        )
    for copy in copies:
        copy.start()
    for copy in copies:
        copy.wait()
    weight = w_ref[...].reshape(D, ROW * C)
    own, left_a, left_b, right_a, right_b, far_a, far_b = tokens
    pieces = (
        (own, 0, 0, 0),
        (own, HALF, 0, HALF),
        (left_a, 0, 3, 0),
        (left_b, 0, 3, HALF),
        (right_a, 0, 1, 0),
        (right_b, 0, 1, HALF),
        (far_a, 0, 2, 0),
        (far_b, 0, 2, HALF),
    )
    for ref, begin, shift, offset in pieces:
        made = jnp.dot(ref[begin : begin + HALF, :], weight, preferred_element_type=f32).astype(bf16)
        row = pl.multiple_of(lax.rem(x + shift, ROW) * POS + offset, HALF)
        act = gelu(made.astype(f32))
        for d in range(ROW):
            part = act[:, d * C : (d + 1) * C]
            center = jnp.mean(part, axis=-1, keepdims=True)
            part = part - center
            spread = jnp.mean(part * part, axis=-1, keepdims=True)
            outs[d][pl.ds(row, HALF), :] = (part * lax.rsqrt(spread + norm_eps)).astype(bf16)


def gate_rows(at, packed, tokens):
    return pl.pallas_call(
        gate_kernel,
        out_shape=[jax.ShapeDtypeStruct((SPAN, C), bf16)] * ROW,
        in_specs=[smem, hbm] + [vmem] * 7,
        out_specs=[vmem] * ROW,
        scratch_shapes=[pltpu.VMEM((DP, K_DEV, ROW * C), bf16), pltpu.SemaphoreType.DMA((ROW,))],
        compiler_params=params(44),
        cost_estimate=pl.CostEstimate(
            flops=2 * SPAN * D * ROW * C, bytes_accessed=10_000_000, transcendentals=SPAN * ROW * C
        ),
        name="gate_rows",
    )(at, packed, *tokens)


def up_kernel(packed_ref, *refs):
    tokens, outs, (w_ref, sems) = refs[:7], refs[7:11], refs[11:]
    copies = []
    for k in range(ROW):
        copies.append(
            pltpu.make_async_copy(
                packed_ref.at[:, PROJ + k * K_DEV : PROJ + (k + 1) * K_DEV, :],
                w_ref.at[:, :, k * C : (k + 1) * C],
                sems.at[k],
            )
        )
    for copy in copies:
        copy.start()
    for copy in copies:
        copy.wait()
    weight = w_ref[...].reshape(D, ROW * C)
    own, left_a, left_b, right_a, right_b, far_a, far_b = tokens
    own_out, left_out, right_out, far_out = outs
    pieces = (
        (far_a, far_out, 0),
        (far_b, far_out, HALF),
        (left_a, left_out, 0),
        (left_b, left_out, HALF),
        (right_a, right_out, 0),
        (right_b, right_out, HALF),
        (own, own_out, None),
    )
    for ref, out, begin in pieces:
        made = jnp.dot(ref[...], weight, preferred_element_type=f32).astype(bf16)
        if begin is None:
            out[...] = made
        else:
            out[begin : begin + HALF, :] = made


def up_rows(packed, tokens):
    return pl.pallas_call(
        up_kernel,
        out_shape=[jax.ShapeDtypeStruct((POS, ROW * C), bf16)] * ROW,
        in_specs=[hbm] + [vmem] * 7,
        out_specs=[vmem] * ROW,
        scratch_shapes=[pltpu.VMEM((DP, K_DEV, ROW * C), bf16), pltpu.SemaphoreType.DMA((ROW,))],
        compiler_params=params(44),
        cost_estimate=pl.CostEstimate(flops=2 * SPAN * D * ROW * C, bytes_accessed=10_000_000, transcendentals=0),
        name="up_rows",
    )(packed, *tokens)


def mix_kernel(at_ref, packed_ref, gain_ref, bias_ref, *refs):
    nv, (out_ref, m_ref, sems) = refs[:ROW], refs[ROW:]
    copies = []
    for k in range(SPAN // C):
        begin = 2 * PROJ + k * M_DEV
        copies.append(
            pltpu.make_async_copy(
                packed_ref.at[:, begin : begin + M_DEV, :], m_ref.at[:, :, k * C : (k + 1) * C], sems.at[k]
            )
        )
    for copy in copies:
        copy.start()
    bias = jnp.broadcast_to(bias_ref[...], (C, SPAN)).T
    gain = gain_ref[...]
    y = at_ref[0]
    for copy in copies:
        copy.wait()
    values = jnp.concatenate([ref[...] for ref in nv], axis=1)
    per = POS // M_DEV
    for t in range(ROW):
        width = -(-(t + 1) * POS // C) * C
        rows = m_ref[t * per : (t + 1) * per, :, :width].reshape(POS, width)
        i = lax.broadcasted_iota(jnp.int32, (POS, width), 0) + t * POS
        j = lax.broadcasted_iota(jnp.int32, (POS, width), 1)
        rows = jnp.where(j <= i, rows, jnp.zeros_like(rows))
        made = jnp.dot(rows, values[:width, :], preferred_element_type=f32)
        for d in range(ROW):
            block = lax.rem(y + ROW - d, ROW)
            part = made[:, d * C : (d + 1) * C] * gain + bias[t * POS : (t + 1) * POS, :]
            out_ref[block * ROW + t] = part.astype(bf16)


def mix(at, packed, gain, bias, nv):
    return pl.pallas_call(
        mix_kernel,
        out_shape=jax.ShapeDtypeStruct((ROW * ROW, POS, C), bf16),
        in_specs=[smem, hbm] + [vmem] * 6,
        out_specs=vmem,
        scratch_shapes=[pltpu.VMEM((DP, M_DEV, SPAN), bf16), pltpu.SemaphoreType.DMA((SPAN // C,))],
        compiler_params=params(47),
        cost_estimate=pl.CostEstimate(flops=2 * SPAN * SPAN * ROW * C, bytes_accessed=7_000_000, transcendentals=0),
        name="mix_positions",
    )(at, packed, gain, bias, *nv)


def open_kernel(at_ref, *refs):
    up, out_ref = refs[:ROW], refs[ROW]
    x = at_ref[1]
    for e in range(ROW):
        source = lax.rem(x + ROW - e, ROW)
        for k in range(ROW):
            out_ref[k * ROW + source] = gelu(up[e][:, k * C : (k + 1) * C].astype(f32))


def open_rows(at, up):
    return pl.pallas_call(
        open_kernel,
        out_shape=jax.ShapeDtypeStruct((ROW * ROW, POS, C), f32),
        in_specs=[smem] + [vmem] * ROW,
        out_specs=vmem,
        compiler_params=params(12),
        cost_estimate=pl.CostEstimate(flops=POS * D * 10, bytes_accessed=4_000_000, transcendentals=POS * D),
        name="open_rows",
    )(at, *up)


def out_kernel(mixed_ref, opened_ref, gain_ref, blocks_ref, out_ref, gated_ref, w_ref, sems):
    steps = DP // 2
    copies = [
        pltpu.make_async_copy(blocks_ref.at[2 * n : 2 * n + 2], w_ref.at[2 * n : 2 * n + 2], sems.at[n])
        for n in range(steps)
    ]
    for copy in copies:
        copy.start()
    total = jnp.zeros((POS, C), f32)
    for g in range(ROW * ROW):
        cols = slice(g * C, (g + 1) * C)
        gated = (opened_ref[g] * mixed_ref[g].astype(f32)).astype(bf16).astype(f32)
        gated_ref[:, cols] = (gated * gain_ref[:, cols]).astype(bf16)
        total = total + gated * gated
    scale = lax.rsqrt(jnp.sum(total, axis=-1, keepdims=True) / D + norm_eps)
    for n in range(steps):
        copies[n].wait()
        weight = jnp.concatenate([w_ref[2 * n], w_ref[2 * n + 1]], axis=1)
        made = jnp.dot(gated_ref[...], weight, preferred_element_type=f32)
        out_ref[:, 2 * n * K_DEV : 2 * (n + 1) * K_DEV] = (made * scale).astype(bf16)


def out_project(mixed, opened, gain, blocks):
    return pl.pallas_call(
        out_kernel,
        out_shape=jax.ShapeDtypeStruct((POS, D), bf16),
        in_specs=[vmem, vmem, vmem, hbm],
        out_specs=vmem,
        scratch_shapes=[
            pltpu.VMEM((POS, D), bf16),
            pltpu.VMEM((DP, D, K_DEV), bf16),
            pltpu.SemaphoreType.DMA((DP // 2,)),
        ],
        compiler_params=params(45),
        cost_estimate=pl.CostEstimate(flops=2 * POS * D * D, bytes_accessed=13_000_000, transcendentals=0),
        name="norm_out",
    )(mixed, opened, gain, blocks)


def body(tokens, up_weight, gate_weight, group_gain, mix_weight, mix_bias, out_gain, out_weight):
    own = tokens[0]
    place = lax.axis_index("sp").astype(jnp.int32)
    at = jnp.stack([lax.div(place, ROW), lax.rem(place, ROW)])
    packed_own = pl.pallas_call(
        pack_kernel,
        out_shape=jax.ShapeDtypeStruct((PACK, C), bf16),
        in_specs=[smem, hbm, hbm, hbm],
        out_specs=hbm,
        scratch_shapes=[pltpu.SemaphoreType.DMA((2 * ROW + SPAN // C,))],
        compiler_params=params(56),
        name="pack_rows",
    )(at, gate_weight, up_weight, mix_weight[0])
    packed = lax.all_gather(packed_own, "dp")
    out_shard, _ = lax.optimization_barrier((out_weight, packed_own))
    out_blocks = lax.all_gather(out_shard, "dp")

    head, tail = own[:HALF], own[HALF:]
    left_a = lax.ppermute(head, "sp", along_x)
    right_b = lax.ppermute(tail, "sp", against_x)
    left_b = lax.ppermute(tail, "sp", along_x)
    right_a = lax.ppermute(head, "sp", against_x)
    far_a = lax.ppermute(left_a, "sp", along_x)
    far_b = lax.ppermute(right_b, "sp", against_x)
    rows = (own, left_a, left_b, right_a, right_b, far_a, far_b)

    nv = list(gate_rows(at, packed, rows))
    for d, p in ((2, across_y), (1, along_y), (3, against_y)):
        nv[d] = lax.ppermute(nv[d], "sp", p)
    made = up_rows(packed, rows)
    up = [made[0]]
    for n, p in ((2, along_x), (3, across_x), (1, against_x)):
        up.append(lax.ppermute(made[n], "sp", p))
    mixed = mix(at, packed, group_gain, mix_bias, nv)
    mixed = lax.all_to_all(mixed, "sp", split_axis=0, concat_axis=0, tiled=True)
    opened = open_rows(at, up)
    return out_project(mixed, opened, out_gain.reshape(1, D), out_blocks)[None]


def solution(mesh):
    return jax.shard_map(
        body,
        mesh=mesh,
        in_specs=(
            P("dp", "sp", None),
            P("dp", None),
            P("dp", None),
            P("sp", None),
            P("sp", "dp", None),
            P("sp", None),
            P(),
            P(None, "dp"),
        ),
        out_specs=P("dp", "sp", None),
        check_vma=False,
    )
```

```python
import jax
import jax.numpy as jnp
from jax import lax
from jax.experimental import pallas as pl
from jax.experimental.pallas import tpu as pltpu
from jax.sharding import PartitionSpec as P


norm_eps = 1e-06
bf16 = jnp.bfloat16
f32 = jnp.float32

ROW = 4
DP = 16
C = 128
POS = 320
HALF = POS // 2
SPAN = 1280
D = 2048
K_DEV = D // DP
M_DEV = SPAN // DP
PROJ = ROW * K_DEV
PACK = 2 * PROJ
CHIPS = DP // 2
CUT = PACK // 2

along_x = [(y * 4 + x, y * 4 + (x + 1) % 4) for y in range(4) for x in range(4)]
against_x = [(b, a) for a, b in along_x]
across_x = [(y * 4 + x, y * 4 + (x + 2) % 4) for y in range(4) for x in range(4)]
along_y = [(y * 4 + x, (y + 1) % 4 * 4 + x) for y in range(4) for x in range(4)]
against_y = [(b, a) for a, b in along_y]
across_y = [(y * 4 + x, (y + 2) % 4 * 4 + x) for y in range(4) for x in range(4)]

along_z = [(2 * z + c, (2 * z + 2) % DP + c) for z in range(CHIPS) for c in range(2)]
against_z = [(b, a) for a, b in along_z]
partner = [(d, d ^ 1) for d in range(DP)]

vmem = pl.BlockSpec(memory_space=pltpu.VMEM)
hbm = pl.BlockSpec(memory_space=pltpu.HBM)


def params(mib):
    return pltpu.CompilerParams(vmem_limit_bytes=mib * 1024 * 1024)


def x_of():
    return lax.rem(lax.axis_index("sp"), ROW)


def y_of():
    return lax.div(lax.axis_index("sp"), ROW)


def pack_kernel(gate_ref, up_ref, out_ref):
    x = x_of()
    for k in range(ROW):
        col = pl.multiple_of((ROW * k + x) * C, C)
        out_ref[k * K_DEV : (k + 1) * K_DEV, :] = gate_ref[:, pl.ds(col, C)]
        out_ref[PROJ + k * K_DEV : PROJ + (k + 1) * K_DEV, :] = up_ref[:, pl.ds(col, C)]


def assemble_kernel(*refs):
    shards, (far_a, far_b), out_ref = refs[:7], refs[7:9], refs[9]
    z = lax.div(lax.axis_index("dp"), 2)
    for ref, back in zip(shards, (0, 1, -1, 2, -2, 3, -3)):
        out_ref[lax.rem(z + CHIPS - back, CHIPS)] = ref[...]
    far = lax.rem(z + CHIPS // 2, CHIPS)
    out_ref[far, :CUT, :] = far_a[...]
    out_ref[far, CUT:, :] = far_b[...]


def assemble(shards):
    return pl.pallas_call(
        assemble_kernel,
        out_shape=jax.ShapeDtypeStruct((CHIPS, PACK, C), bf16),
        in_specs=[vmem] * 9,
        out_specs=vmem,
        compiler_params=params(8),
        cost_estimate=pl.CostEstimate(flops=1_000_000, bytes_accessed=4_200_000, transcendentals=0),
        name="assemble_rows",
    )(*shards)


def gelu(v):
    return jax.nn.gelu(v, approximate=True)


def lay_weight(own_ref, other_ref, blocks, w_ref):
    core = lax.rem(lax.axis_index("dp"), 2)
    for n, begin in enumerate(blocks):
        for ref, place in ((own_ref, core), (other_ref, 1 - core)):
            for z in range(CHIPS):
                w_ref[z, place, :, n * C : (n + 1) * C] = ref[z, pl.ds(begin, K_DEV), :]
    return w_ref[...].reshape(D, ROW * C)


def row_pieces(tokens):
    own, left_a, left_b, right_a, right_b, far_a, far_b = tokens
    yield own[...]
    for a, b in ((left_a, left_b), (right_a, right_b), (far_a, far_b)):
        yield jnp.concatenate([a[...], b[...]], axis=0)


def gate_kernel(own_ref, other_ref, *refs):
    tokens, outs, w_ref = refs[:7], refs[7:11], refs[11]
    y = y_of()
    x = x_of()
    blocks = [pl.multiple_of(lax.rem(y + d, ROW) * K_DEV, K_DEV) for d in range(ROW)]
    weight = lay_weight(own_ref, other_ref, blocks, w_ref)
    for piece, shift in zip(row_pieces(tokens), (0, 3, 1, 2)):
        made = jnp.dot(piece, weight, preferred_element_type=f32).astype(bf16)
        row = pl.multiple_of(lax.rem(x + shift, ROW) * POS, POS)
        act = gelu(made.astype(f32))
        for d in range(ROW):
            part = act[:, d * C : (d + 1) * C]
            center = jnp.mean(part, axis=-1, keepdims=True)
            part = part - center
            spread = jnp.mean(part * part, axis=-1, keepdims=True)
            outs[d][pl.ds(row, POS), :] = (part * lax.rsqrt(spread + norm_eps)).astype(bf16)


def up_kernel(own_ref, other_ref, *refs):
    tokens, outs, w_ref = refs[:7], refs[7:11], refs[11]
    weight = lay_weight(own_ref, other_ref, [PROJ + k * K_DEV for k in range(ROW)], w_ref)
    for piece, out in zip(row_pieces(tokens), outs):
        out[...] = jnp.dot(piece, weight, preferred_element_type=f32).astype(bf16)


def project(kernel, shape, transcendentals, own, other, tokens):
    return pl.pallas_call(
        kernel,
        out_shape=[jax.ShapeDtypeStruct(shape, bf16)] * ROW,
        in_specs=[vmem] * 9,
        out_specs=[vmem] * ROW,
        scratch_shapes=[pltpu.VMEM((CHIPS, 2, K_DEV, ROW * C), bf16)],
        compiler_params=params(24),
        cost_estimate=pl.CostEstimate(
            flops=2 * SPAN * D * ROW * C, bytes_accessed=10_000_000, transcendentals=transcendentals
        ),
    )(own, other, *tokens)


def gate_rows(own, other, tokens):
    return project(gate_kernel, (SPAN, C), SPAN * ROW * C, own, other, tokens)


def up_rows(own, other, tokens):
    return project(up_kernel, (POS, ROW * C), 0, own, other, tokens)


WIDTHS = [-(-(t + 1) * POS // C) * C for t in range(ROW)]


def lower_kernel(rows_ref, out_ref, m_ref, sems):
    per = POS // M_DEV
    copies = []
    for t, width in enumerate(WIDTHS):
        part = (slice(t * per, (t + 1) * per), slice(None), slice(0, width))
        copies.append(pltpu.make_async_copy(rows_ref.at[part], m_ref.at[part], sems.at[t]))
        copies[t].start()
    for t, width in enumerate(WIDTHS):
        copies[t].wait()
        rows = m_ref[t * per : (t + 1) * per, :, :width].reshape(POS, width)
        i = lax.broadcasted_iota(jnp.int32, (POS, width), 0) + t * POS
        j = lax.broadcasted_iota(jnp.int32, (POS, width), 1)
        out_ref[t * POS : (t + 1) * POS, :width] = jnp.where(j <= i, rows, jnp.zeros_like(rows))


def lower_rows(rows):
    return pl.pallas_call(
        lower_kernel,
        out_shape=jax.ShapeDtypeStruct((SPAN, SPAN), bf16),
        in_specs=[hbm],
        out_specs=vmem,
        scratch_shapes=[pltpu.VMEM((DP, M_DEV, SPAN), bf16), pltpu.SemaphoreType.DMA((ROW,))],
        compiler_params=params(48),
        cost_estimate=pl.CostEstimate(flops=2_000_000, bytes_accessed=6_000_000, transcendentals=0),
        name="lower_rows",
    )(rows)


def mix_kernel(lower_ref, gain_ref, bias_ref, *refs):
    nv, out_ref = refs[:ROW], refs[ROW]
    y = y_of()
    gain = gain_ref[...]
    bias = jnp.broadcast_to(bias_ref[...], (C, SPAN)).T
    values = jnp.concatenate([ref[...] for ref in nv], axis=1)
    for t, width in enumerate(WIDTHS):
        rows = lower_ref[t * POS : (t + 1) * POS, :width]
        made = jnp.dot(rows, values[:width, :], preferred_element_type=f32)
        for d in range(ROW):
            block = lax.rem(y + ROW - d, ROW)
            part = made[:, d * C : (d + 1) * C] * gain + bias[t * POS : (t + 1) * POS, :]
            out_ref[block * ROW + t] = part.astype(bf16)


def mix(lower, gain, bias, nv):
    return pl.pallas_call(
        mix_kernel,
        out_shape=jax.ShapeDtypeStruct((ROW * ROW, POS, C), bf16),
        in_specs=[vmem] * 7,
        out_specs=vmem,
        compiler_params=params(16),
        cost_estimate=pl.CostEstimate(flops=2 * SPAN * SPAN * ROW * C, bytes_accessed=7_000_000, transcendentals=0),
        name="mix_positions",
    )(lower, gain, bias, *nv)


def open_kernel(*refs):
    up, out_ref = refs[:ROW], refs[ROW]
    x = x_of()
    for e in range(ROW):
        source = lax.rem(x + ROW - e, ROW)
        for k in range(ROW):
            out_ref[k * ROW + source] = gelu(up[e][:, k * C : (k + 1) * C].astype(f32))


def open_rows(up):
    return pl.pallas_call(
        open_kernel,
        out_shape=jax.ShapeDtypeStruct((ROW * ROW, POS, C), f32),
        in_specs=[vmem] * ROW,
        out_specs=vmem,
        compiler_params=params(12),
        cost_estimate=pl.CostEstimate(flops=POS * D * 10, bytes_accessed=4_000_000, transcendentals=POS * D),
        name="open_rows",
    )(*up)


def out_kernel(mixed_ref, opened_ref, gain_ref, blocks_ref, out_ref, gated_ref, w_ref, sems):
    steps = DP // 4
    copies = [
        pltpu.make_async_copy(blocks_ref.at[4 * n : 4 * n + 4], w_ref.at[4 * n : 4 * n + 4], sems.at[n])
        for n in range(steps)
    ]
    for copy in copies:
        copy.start()
    total = jnp.zeros((POS, C), f32)
    for g in range(ROW * ROW):
        cols = slice(g * C, (g + 1) * C)
        gated = (opened_ref[g] * mixed_ref[g].astype(f32)).astype(bf16).astype(f32)
        gated_ref[:, cols] = (gated * gain_ref[:, cols]).astype(bf16)
        total = total + gated * gated
    scale = lax.rsqrt(jnp.sum(total, axis=-1, keepdims=True) / D + norm_eps)
    for n in range(steps):
        copies[n].wait()
        weight = jnp.concatenate([w_ref[4 * n + k] for k in range(4)], axis=1)
        made = jnp.dot(gated_ref[...], weight, preferred_element_type=f32)
        out_ref[:, 4 * n * K_DEV : 4 * (n + 1) * K_DEV] = (made * scale).astype(bf16)


def out_project(mixed, opened, gain, blocks):
    return pl.pallas_call(
        out_kernel,
        out_shape=jax.ShapeDtypeStruct((POS, D), bf16),
        in_specs=[vmem, vmem, vmem, hbm],
        out_specs=vmem,
        scratch_shapes=[
            pltpu.VMEM((POS, D), bf16),
            pltpu.VMEM((DP, D, K_DEV), bf16),
            pltpu.SemaphoreType.DMA((DP // 4,)),
        ],
        compiler_params=params(45),
        cost_estimate=pl.CostEstimate(flops=2 * POS * D * D, bytes_accessed=13_000_000, transcendentals=0),
        name="norm_out",
    )(mixed, opened, gain, blocks)


def body(tokens, up_weight, gate_weight, group_gain, mix_weight, mix_bias, out_gain, out_weight):
    own = tokens[0]

    packed_own = pl.pallas_call(
        pack_kernel,
        out_shape=jax.ShapeDtypeStruct((PACK, C), bf16),
        in_specs=[vmem, vmem],
        out_specs=vmem,
        compiler_params=params(56),
        name="pack_rows",
    )(gate_weight, up_weight)
    mix_rows = lax.all_gather(mix_weight[0], "dp")
    out_blocks = lax.all_gather(out_weight, "dp")

    one_p = lax.ppermute(packed_own, "dp", along_z)
    one_m = lax.ppermute(packed_own, "dp", against_z)
    head, tail = own[:HALF], own[HALF:]
    left_a = lax.ppermute(head, "sp", along_x)
    right_b = lax.ppermute(tail, "sp", against_x)
    left_b = lax.ppermute(tail, "sp", along_x)
    right_a = lax.ppermute(head, "sp", against_x)
    two_p = lax.ppermute(one_p, "dp", along_z)
    two_m = lax.ppermute(one_m, "dp", against_z)
    three_p = lax.ppermute(two_p, "dp", along_z)
    three_m = lax.ppermute(two_m, "dp", against_z)
    far_a = lax.ppermute(left_a, "sp", along_x)
    far_b = lax.ppermute(right_b, "sp", against_x)
    four_p = lax.ppermute(three_p[:CUT], "dp", along_z)
    four_m = lax.ppermute(three_m[CUT:], "dp", against_z)
    own_w = assemble((packed_own, one_p, one_m, two_p, two_m, three_p, three_m, four_p, four_m))
    other_w = lax.ppermute(own_w, "dp", partner)
    rows = (own, left_a, left_b, right_a, right_b, far_a, far_b)

    nv = list(gate_rows(own_w, other_w, rows))
    for d, p in ((2, across_y), (1, along_y), (3, against_y)):
        nv[d] = lax.ppermute(nv[d], "sp", p)
    made = up_rows(own_w, other_w, rows)
    up = [made[0]]
    for n, p in ((2, along_x), (3, across_x), (1, against_x)):
        up.append(lax.ppermute(made[n], "sp", p))
    lower = lower_rows(mix_rows)
    mixed = mix(lower, group_gain, mix_bias, nv)
    mixed = lax.all_to_all(mixed, "sp", split_axis=0, concat_axis=0, tiled=True)
    opened = open_rows(up)
    return out_project(mixed, opened, out_gain.reshape(1, D), out_blocks)[None]


def solution(mesh):
    return jax.shard_map(
        body,
        mesh=mesh,
        in_specs=(
            P("dp", "sp", None),
            P("dp", None),
            P("dp", None),
            P("sp", None),
            P("sp", "dp", None),
            P("sp", None),
            P(),
            P(None, "dp"),
        ),
        out_specs=P("dp", "sp", None),
        check_vma=False,
    )
```

```python
import jax
import jax.numpy as jnp
from jax import lax
from jax.experimental import pallas as pl
from jax.experimental.pallas import tpu as pltpu
from jax.sharding import PartitionSpec as P


norm_eps = 1e-06
bf16 = jnp.bfloat16
f32 = jnp.float32

ROW = 4
DP = 16
C = 128
POS = 320
HALF = POS // 2
SPAN = 1280
D = 2048
K_DEV = D // DP
M_DEV = SPAN // DP
PROJ = ROW * K_DEV
PACK = 2 * PROJ
CHIPS = DP // 2
CUT = PACK // 2

along_x = [(y * 4 + x, y * 4 + (x + 1) % 4) for y in range(4) for x in range(4)]
against_x = [(b, a) for a, b in along_x]
across_x = [(y * 4 + x, y * 4 + (x + 2) % 4) for y in range(4) for x in range(4)]
along_y = [(y * 4 + x, (y + 1) % 4 * 4 + x) for y in range(4) for x in range(4)]
against_y = [(b, a) for a, b in along_y]
across_y = [(y * 4 + x, (y + 2) % 4 * 4 + x) for y in range(4) for x in range(4)]

along_z = [(2 * z + c, (2 * z + 2) % DP + c) for z in range(CHIPS) for c in range(2)]
against_z = [(b, a) for a, b in along_z]
partner = [(d, d ^ 1) for d in range(DP)]

vmem = pl.BlockSpec(memory_space=pltpu.VMEM)
hbm = pl.BlockSpec(memory_space=pltpu.HBM)


def params(mib):
    return pltpu.CompilerParams(vmem_limit_bytes=mib * 1024 * 1024)


def x_of():
    return lax.rem(lax.axis_index("sp"), ROW)


def y_of():
    return lax.div(lax.axis_index("sp"), ROW)


def pack_kernel(gate_ref, up_ref, out_ref):
    x = x_of()
    for k in range(ROW):
        col = pl.multiple_of((ROW * k + x) * C, C)
        out_ref[k * K_DEV : (k + 1) * K_DEV, :] = gate_ref[:, pl.ds(col, C)]
        out_ref[PROJ + k * K_DEV : PROJ + (k + 1) * K_DEV, :] = up_ref[:, pl.ds(col, C)]


def join_kernel(*refs):
    *shards, out_ref = refs
    row = 0
    for ref in shards:
        slot, begin = divmod(row, PACK)
        out_ref[slot, begin : begin + ref.shape[0], :] = ref[...]
        row += ref.shape[0]


def join(shards):
    count = sum(shard.shape[0] for shard in shards) // PACK
    return pl.pallas_call(
        join_kernel,
        out_shape=jax.ShapeDtypeStruct((count, PACK, C), bf16),
        in_specs=[vmem] * len(shards),
        out_specs=vmem,
        compiler_params=params(8),
        cost_estimate=pl.CostEstimate(flops=1_000_000, bytes_accessed=3_000_000, transcendentals=0),
        name="join_shards",
    )(*shards)


def gelu(v):
    return jax.nn.gelu(v, approximate=True)


NEAR = (0, 1, -1, 2, -2)
FAR = (3, -3, 4)


def lay_weight(parts, blocks, w_ref):
    dp = lax.axis_index("dp")
    z = lax.div(dp, 2)
    core = lax.rem(dp, 2)
    near, far, other_near, other_far = parts
    for ref, backs, place in (
        (near, NEAR, core),
        (far, FAR, core),
        (other_near, NEAR, 1 - core),
        (other_far, FAR, 1 - core),
    ):
        for k, back in enumerate(backs):
            chip = lax.rem(z + CHIPS - back, CHIPS)
            for n, begin in enumerate(blocks):
                w_ref[chip, place, :, n * C : (n + 1) * C] = ref[k, pl.ds(begin, K_DEV), :]
    return w_ref[...].reshape(D, ROW * C)


def row_pieces(tokens):
    own, left, right, far_a, far_b = tokens
    yield from (own[...], left[...], right[...])
    yield jnp.concatenate([far_a[...], far_b[...]], axis=0)


def gate_kernel(*refs):
    parts, tokens, outs, w_ref = refs[:4], refs[4:9], refs[9:13], refs[13]
    y = y_of()
    x = x_of()
    blocks = [pl.multiple_of(lax.rem(y + d, ROW) * K_DEV, K_DEV) for d in range(ROW)]
    weight = lay_weight(parts, blocks, w_ref)
    for piece, shift in zip(row_pieces(tokens), (0, 3, 1, 2)):
        made = jnp.dot(piece, weight, preferred_element_type=f32).astype(bf16)
        row = pl.multiple_of(lax.rem(x + shift, ROW) * POS, POS)
        act = gelu(made.astype(f32))
        for d in range(ROW):
            part = act[:, d * C : (d + 1) * C]
            center = jnp.mean(part, axis=-1, keepdims=True)
            part = part - center
            spread = jnp.mean(part * part, axis=-1, keepdims=True)
            outs[d][pl.ds(row, POS), :] = (part * lax.rsqrt(spread + norm_eps)).astype(bf16)


def up_kernel(*refs):
    parts, tokens, outs, w_ref = refs[:4], refs[4:9], refs[9:13], refs[13]
    weight = lay_weight(parts, [PROJ + k * K_DEV for k in range(ROW)], w_ref)
    for piece, out in zip(row_pieces(tokens), outs):
        out[...] = jnp.dot(piece, weight, preferred_element_type=f32).astype(bf16)


def project(kernel, shape, transcendentals, parts, tokens):
    return pl.pallas_call(
        kernel,
        out_shape=[jax.ShapeDtypeStruct(shape, bf16)] * ROW,
        in_specs=[vmem] * 9,
        out_specs=[vmem] * ROW,
        scratch_shapes=[pltpu.VMEM((CHIPS, 2, K_DEV, ROW * C), bf16)],
        compiler_params=params(24),
        cost_estimate=pl.CostEstimate(
            flops=2 * SPAN * D * ROW * C, bytes_accessed=10_000_000, transcendentals=transcendentals
        ),
    )(*parts, *tokens)


def gate_rows(parts, tokens):
    return project(gate_kernel, (SPAN, C), SPAN * ROW * C, parts, tokens)


def up_rows(parts, tokens):
    return project(up_kernel, (POS, ROW * C), 0, parts, tokens)


WIDTHS = [-(-(t + 1) * POS // C) * C for t in range(ROW)]


def lower_kernel(rows_ref, out_ref, m_ref, sems):
    per = POS // M_DEV
    copies = []
    for t, width in enumerate(WIDTHS):
        part = (slice(t * per, (t + 1) * per), slice(None), slice(0, width))
        copies.append(pltpu.make_async_copy(rows_ref.at[part], m_ref.at[part], sems.at[t]))
        copies[t].start()
    for t, width in enumerate(WIDTHS):
        copies[t].wait()
        rows = m_ref[t * per : (t + 1) * per, :, :width].reshape(POS, width)
        i = lax.broadcasted_iota(jnp.int32, (POS, width), 0) + t * POS
        j = lax.broadcasted_iota(jnp.int32, (POS, width), 1)
        out_ref[t * POS : (t + 1) * POS, :width] = jnp.where(j <= i, rows, jnp.zeros_like(rows))


def lower_rows(rows):
    return pl.pallas_call(
        lower_kernel,
        out_shape=jax.ShapeDtypeStruct((SPAN, SPAN), bf16),
        in_specs=[hbm],
        out_specs=vmem,
        scratch_shapes=[pltpu.VMEM((DP, M_DEV, SPAN), bf16), pltpu.SemaphoreType.DMA((ROW,))],
        compiler_params=params(48),
        cost_estimate=pl.CostEstimate(flops=2_000_000, bytes_accessed=6_000_000, transcendentals=0),
        name="lower_rows",
    )(rows)


def mix_kernel(lower_ref, gain_ref, bias_ref, *refs):
    nv, out_ref = refs[:ROW], refs[ROW]
    y = y_of()
    gain = gain_ref[...]
    bias = jnp.broadcast_to(bias_ref[...], (C, SPAN)).T
    values = jnp.concatenate([ref[...] for ref in nv], axis=1)
    for t, width in enumerate(WIDTHS):
        rows = lower_ref[t * POS : (t + 1) * POS, :width]
        made = jnp.dot(rows, values[:width, :], preferred_element_type=f32)
        for d in range(ROW):
            block = lax.rem(y + ROW - d, ROW)
            part = made[:, d * C : (d + 1) * C] * gain + bias[t * POS : (t + 1) * POS, :]
            out_ref[block * ROW + t] = part.astype(bf16)


def mix(lower, gain, bias, nv):
    return pl.pallas_call(
        mix_kernel,
        out_shape=jax.ShapeDtypeStruct((ROW * ROW, POS, C), bf16),
        in_specs=[vmem] * 7,
        out_specs=vmem,
        compiler_params=params(16),
        cost_estimate=pl.CostEstimate(flops=2 * SPAN * SPAN * ROW * C, bytes_accessed=7_000_000, transcendentals=0),
        name="mix_positions",
    )(lower, gain, bias, *nv)


def open_kernel(*refs):
    up, out_ref = refs[:ROW], refs[ROW]
    x = x_of()
    for e in range(ROW):
        source = lax.rem(x + ROW - e, ROW)
        for k in range(ROW):
            out_ref[k * ROW + source] = gelu(up[e][:, k * C : (k + 1) * C].astype(f32))


def open_rows(up):
    return pl.pallas_call(
        open_kernel,
        out_shape=jax.ShapeDtypeStruct((ROW * ROW, POS, C), f32),
        in_specs=[vmem] * ROW,
        out_specs=vmem,
        compiler_params=params(12),
        cost_estimate=pl.CostEstimate(flops=POS * D * 10, bytes_accessed=4_000_000, transcendentals=POS * D),
        name="open_rows",
    )(*up)


def out_kernel(mixed_ref, opened_ref, gain_ref, blocks_ref, out_ref, gated_ref, w_ref, sems):
    steps = DP // 4
    copies = [
        pltpu.make_async_copy(blocks_ref.at[4 * n : 4 * n + 4], w_ref.at[4 * n : 4 * n + 4], sems.at[n])
        for n in range(steps)
    ]
    for copy in copies:
        copy.start()
    total = jnp.zeros((POS, C), f32)
    for g in range(ROW * ROW):
        cols = slice(g * C, (g + 1) * C)
        gated = (opened_ref[g] * mixed_ref[g].astype(f32)).astype(bf16).astype(f32)
        gated_ref[:, cols] = (gated * gain_ref[:, cols]).astype(bf16)
        total = total + gated * gated
    scale = lax.rsqrt(jnp.sum(total, axis=-1, keepdims=True) / D + norm_eps)
    for n in range(steps):
        copies[n].wait()
        weight = jnp.concatenate([w_ref[4 * n + k] for k in range(4)], axis=1)
        made = jnp.dot(gated_ref[...], weight, preferred_element_type=f32)
        out_ref[:, 4 * n * K_DEV : 4 * (n + 1) * K_DEV] = (made * scale).astype(bf16)


def out_project(mixed, opened, gain, blocks):
    return pl.pallas_call(
        out_kernel,
        out_shape=jax.ShapeDtypeStruct((POS, D), bf16),
        in_specs=[vmem, vmem, vmem, hbm],
        out_specs=vmem,
        scratch_shapes=[
            pltpu.VMEM((POS, D), bf16),
            pltpu.VMEM((DP, D, K_DEV), bf16),
            pltpu.SemaphoreType.DMA((DP // 4,)),
        ],
        compiler_params=params(45),
        cost_estimate=pl.CostEstimate(flops=2 * POS * D * D, bytes_accessed=13_000_000, transcendentals=0),
        name="norm_out",
    )(mixed, opened, gain, blocks)


def body(tokens, up_weight, gate_weight, group_gain, mix_weight, mix_bias, out_gain, out_weight):
    own = tokens[0]

    packed_own = pl.pallas_call(
        pack_kernel,
        out_shape=jax.ShapeDtypeStruct((PACK, C), bf16),
        in_specs=[vmem, vmem],
        out_specs=vmem,
        compiler_params=params(56),
        name="pack_rows",
    )(gate_weight, up_weight)
    mix_shard, out_shard, _ = lax.optimization_barrier((mix_weight[0], out_weight, packed_own))
    mix_rows = lax.all_gather(mix_shard, "dp")
    out_blocks = lax.all_gather(out_shard, "dp")

    one_p = lax.ppermute(packed_own, "dp", along_z)
    one_m = lax.ppermute(packed_own, "dp", against_z)
    left = lax.ppermute(own, "sp", along_x)
    right = lax.ppermute(own, "sp", against_x)
    two_p = lax.ppermute(one_p, "dp", along_z)
    two_m = lax.ppermute(one_m, "dp", against_z)
    three_p = lax.ppermute(two_p, "dp", along_z)
    three_m = lax.ppermute(two_m, "dp", against_z)
    near = join((packed_own, one_p, one_m, two_p, two_m))
    other_near = lax.ppermute(near, "dp", partner)
    far_a = lax.ppermute(left[:HALF], "sp", along_x)
    far_b = lax.ppermute(right[HALF:], "sp", against_x)
    four_p = lax.ppermute(three_p[:CUT], "dp", along_z)
    four_m = lax.ppermute(three_m[CUT:], "dp", against_z)
    far = join((three_p, three_m, four_p, four_m))
    other_far = lax.ppermute(far, "dp", partner)
    parts = (near, far, other_near, other_far)
    rows = (own, left, right, far_a, far_b)

    nv = list(gate_rows(parts, rows))
    for d, p in ((2, across_y), (1, along_y), (3, against_y)):
        nv[d] = lax.ppermute(nv[d], "sp", p)
    made = up_rows(parts, rows)
    up = [made[0]]
    for n, p in ((2, along_x), (3, across_x), (1, against_x)):
        up.append(lax.ppermute(made[n], "sp", p))
    lower = lower_rows(mix_rows)
    mixed = mix(lower, group_gain, mix_bias, nv)
    mixed = lax.all_to_all(mixed, "sp", split_axis=0, concat_axis=0, tiled=True)
    opened = open_rows(up)
    return out_project(mixed, opened, out_gain.reshape(1, D), out_blocks)[None]


def solution(mesh):
    return jax.shard_map(
        body,
        mesh=mesh,
        in_specs=(
            P("dp", "sp", None),
            P("dp", None),
            P("dp", None),
            P("sp", None),
            P("sp", "dp", None),
            P("sp", None),
            P(),
            P(None, "dp"),
        ),
        out_specs=P("dp", "sp", None),
        check_vma=False,
    )
```

```python
import jax
import jax.numpy as jnp
from jax import lax
from jax.experimental import pallas as pl
from jax.experimental.pallas import tpu as pltpu
from jax.sharding import PartitionSpec as P


norm_eps = 1e-06
bf16 = jnp.bfloat16
f32 = jnp.float32

ROW = 4
DP = 16
C = 128
POS = 320
HALF = POS // 2
SPAN = 1280
D = 2048
K_DEV = D // DP
M_DEV = SPAN // DP
PROJ = ROW * K_DEV
PACK = 2 * PROJ
CHIPS = DP // 2
HALF_CHIPS = CHIPS // 2

along_x = [(y * 4 + x, y * 4 + (x + 1) % 4) for y in range(4) for x in range(4)]
against_x = [(b, a) for a, b in along_x]
across_x = [(y * 4 + x, y * 4 + (x + 2) % 4) for y in range(4) for x in range(4)]
along_y = [(y * 4 + x, (y + 1) % 4 * 4 + x) for y in range(4) for x in range(4)]
against_y = [(b, a) for a, b in along_y]
across_y = [(y * 4 + x, (y + 2) % 4 * 4 + x) for y in range(4) for x in range(4)]

along_z = [(2 * z + c, (2 * z + 2) % DP + c) for z in range(CHIPS) for c in range(2)]
against_z = [(b, a) for a, b in along_z]
partner = [(d, d ^ 1) for d in range(DP)]

vmem = pl.BlockSpec(memory_space=pltpu.VMEM)
hbm = pl.BlockSpec(memory_space=pltpu.HBM)


def params(mib):
    return pltpu.CompilerParams(vmem_limit_bytes=mib * 1024 * 1024)


def x_of():
    return lax.rem(lax.axis_index("sp"), ROW)


def y_of():
    return lax.div(lax.axis_index("sp"), ROW)


def pack_kernel(gate_ref, up_ref, out_ref):
    x = x_of()
    for k in range(ROW):
        col = pl.multiple_of((ROW * k + x) * C, C)
        out_ref[k * K_DEV : (k + 1) * K_DEV, :] = gate_ref[:, pl.ds(col, C)]
        out_ref[PROJ + k * K_DEV : PROJ + (k + 1) * K_DEV, :] = up_ref[:, pl.ds(col, C)]


def assemble_kernel(*refs):
    shards, (far_a, far_b), out_ref = refs[:7], refs[7:9], refs[9]
    z = lax.div(lax.axis_index("dp"), 2)
    for ref, back in zip(shards, (0, 1, -1, 2, -2, 3, -3)):
        out_ref[lax.rem(z + CHIPS - back, CHIPS)] = ref[...]
    far = lax.rem(z + HALF_CHIPS, CHIPS)
    cut = far_a.shape[0]
    out_ref[far, :cut, :] = far_a[...]
    out_ref[far, cut:, :] = far_b[...]


def assemble(shards):
    return pl.pallas_call(
        assemble_kernel,
        out_shape=jax.ShapeDtypeStruct((CHIPS,) + shards[0].shape, bf16),
        in_specs=[vmem] * 9,
        out_specs=vmem,
        compiler_params=params(8),
        cost_estimate=pl.CostEstimate(flops=1_000_000, bytes_accessed=4_000_000, transcendentals=0),
        name="assemble",
    )(*shards)


def gelu(v):
    return jax.nn.gelu(v, approximate=True)


def lay_weight(own_ref, other_ref, blocks, w_ref):
    core = lax.rem(lax.axis_index("dp"), 2)

    def lay(z, carry):
        for n, begin in enumerate(blocks):
            for ref, place in ((own_ref, core), (other_ref, 1 - core)):
                w_ref[z, place, :, n * C : (n + 1) * C] = ref[z, pl.ds(begin, K_DEV), :]
        return carry

    lax.fori_loop(0, CHIPS, lay, 0)
    return w_ref[...].reshape(D, ROW * C)


def row_pieces(tokens):
    own, left, right, far_a, far_b = tokens
    yield from (own[...], left[...], right[...])
    yield jnp.concatenate([far_a[...], far_b[...]], axis=0)


def gate_kernel(*refs):
    parts, tokens, outs, w_ref = refs[:2], refs[2:7], refs[7:11], refs[11]
    y = y_of()
    x = x_of()
    blocks = [pl.multiple_of(lax.rem(y + d, ROW) * K_DEV, K_DEV) for d in range(ROW)]
    weight = lay_weight(*parts, blocks, w_ref)
    for piece, shift in zip(row_pieces(tokens), (0, 3, 1, 2)):
        made = jnp.dot(piece, weight, preferred_element_type=f32).astype(bf16)
        row = pl.multiple_of(lax.rem(x + shift, ROW) * POS, POS)
        act = gelu(made.astype(f32))
        for d in range(ROW):
            part = act[:, d * C : (d + 1) * C]
            center = jnp.mean(part, axis=-1, keepdims=True)
            part = part - center
            spread = jnp.mean(part * part, axis=-1, keepdims=True)
            outs[d][pl.ds(row, POS), :] = (part * lax.rsqrt(spread + norm_eps)).astype(bf16)


def up_kernel(*refs):
    parts, tokens, outs, w_ref = refs[:2], refs[2:7], refs[7:11], refs[11]
    weight = lay_weight(*parts, [PROJ + k * K_DEV for k in range(ROW)], w_ref)
    for piece, out in zip(row_pieces(tokens), outs):
        out[...] = jnp.dot(piece, weight, preferred_element_type=f32).astype(bf16)


def project(kernel, shape, transcendentals, parts, tokens):
    return pl.pallas_call(
        kernel,
        out_shape=[jax.ShapeDtypeStruct(shape, bf16)] * ROW,
        in_specs=[vmem] * 7,
        out_specs=[vmem] * ROW,
        scratch_shapes=[pltpu.VMEM((CHIPS, 2, K_DEV, ROW * C), bf16)],
        compiler_params=params(24),
        cost_estimate=pl.CostEstimate(
            flops=2 * SPAN * D * ROW * C, bytes_accessed=10_000_000, transcendentals=transcendentals
        ),
    )(*parts, *tokens)


def gate_rows(parts, tokens):
    return project(gate_kernel, (SPAN, C), SPAN * ROW * C, parts, tokens)


def up_rows(parts, tokens):
    return project(up_kernel, (POS, ROW * C), 0, parts, tokens)


def mix_kernel(own_ref, other_ref, gain_ref, bias_ref, *refs):
    nv, (out_ref, bias_cols) = refs[:ROW], refs[ROW:]
    core = lax.rem(lax.axis_index("dp"), 2)
    y = y_of()
    gain = gain_ref[...]
    bias_cols[...] = jnp.broadcast_to(bias_ref[...], (C, SPAN)).T
    values = jnp.concatenate([ref[...] for ref in nv], axis=1)
    for t in range(ROW):
        width = -(-(t + 1) * POS // C) * C
        begin = t * POS
        parts = ((own_ref, 2 * t, core), (own_ref, 2 * t + 1, core + 2))
        parts += ((other_ref, 2 * t, 1 - core), (other_ref, 2 * t + 1, 3 - core))
        masked = []
        for ref, shard, row in parts:
            rows = ref[shard, :, :width]
            i = lax.broadcasted_iota(jnp.int32, (M_DEV, width), 0) + (begin + row * M_DEV)
            j = lax.broadcasted_iota(jnp.int32, (M_DEV, width), 1)
            masked.append(jnp.where(j <= i, rows, jnp.zeros_like(rows)))
        made = jnp.dot(jnp.concatenate(masked, axis=0), values[:width, :], preferred_element_type=f32)
        for d in range(ROW):
            block = lax.rem(y + ROW - d, ROW)
            for n, (_, _, row) in enumerate(parts):
                at = pl.multiple_of(row * M_DEV, 16)
                part = made[n * M_DEV : (n + 1) * M_DEV, d * C : (d + 1) * C] * gain
                part = part + bias_cols[pl.ds(begin + at, M_DEV), :]
                out_ref[block * ROW + t, pl.ds(at, M_DEV), :] = part.astype(bf16)


def mix(own, other, gain, bias, nv):
    return pl.pallas_call(
        mix_kernel,
        out_shape=jax.ShapeDtypeStruct((ROW * ROW, POS, C), bf16),
        in_specs=[vmem] * 8,
        out_specs=vmem,
        scratch_shapes=[pltpu.VMEM((SPAN, C), f32)],
        compiler_params=params(16),
        cost_estimate=pl.CostEstimate(flops=2 * SPAN * SPAN * ROW * C, bytes_accessed=7_000_000, transcendentals=0),
        name="mix_positions",
    )(own, other, gain, bias, *nv)


def open_kernel(*refs):
    up, out_ref = refs[:ROW], refs[ROW]
    x = x_of()

    def opened(k, carry):
        cols = pl.ds(pl.multiple_of(k * C, C), C)
        for e in range(ROW):
            source = lax.rem(x + ROW - e, ROW)
            out_ref[k * ROW + source] = gelu(up[e][:, cols].astype(f32))
        return carry

    lax.fori_loop(0, ROW, opened, 0)


def open_rows(up):
    return pl.pallas_call(
        open_kernel,
        out_shape=jax.ShapeDtypeStruct((ROW * ROW, POS, C), f32),
        in_specs=[vmem] * ROW,
        out_specs=vmem,
        compiler_params=params(12),
        cost_estimate=pl.CostEstimate(flops=POS * D * 10, bytes_accessed=4_000_000, transcendentals=POS * D),
        name="open_rows",
    )(*up)


def out_kernel(mixed_ref, opened_ref, gain_ref, blocks_ref, out_ref, gated_ref, w_ref, sems):
    steps = DP // 4
    copies = [
        pltpu.make_async_copy(blocks_ref.at[4 * n : 4 * n + 4], w_ref.at[4 * n : 4 * n + 4], sems.at[n])
        for n in range(steps)
    ]
    for copy in copies:
        copy.start()
    total = jnp.zeros((POS, C), f32)
    for g in range(ROW * ROW):
        cols = slice(g * C, (g + 1) * C)
        gated = (opened_ref[g] * mixed_ref[g].astype(f32)).astype(bf16).astype(f32)
        gated_ref[:, cols] = (gated * gain_ref[:, cols]).astype(bf16)
        total = total + gated * gated
    scale = lax.rsqrt(jnp.sum(total, axis=-1, keepdims=True) / D + norm_eps)
    for n in range(steps):
        copies[n].wait()
        weight = jnp.concatenate([w_ref[4 * n + k] for k in range(4)], axis=1)
        made = jnp.dot(gated_ref[...], weight, preferred_element_type=f32)
        out_ref[:, 4 * n * K_DEV : 4 * (n + 1) * K_DEV] = (made * scale).astype(bf16)


def out_project(mixed, opened, gain, blocks):
    return pl.pallas_call(
        out_kernel,
        out_shape=jax.ShapeDtypeStruct((POS, D), bf16),
        in_specs=[vmem, vmem, vmem, hbm],
        out_specs=vmem,
        scratch_shapes=[
            pltpu.VMEM((POS, D), bf16),
            pltpu.VMEM((DP, D, K_DEV), bf16),
            pltpu.SemaphoreType.DMA((DP // 4,)),
        ],
        compiler_params=params(45),
        cost_estimate=pl.CostEstimate(flops=2 * POS * D * D, bytes_accessed=13_000_000, transcendentals=0),
        name="norm_out",
    )(mixed, opened, gain, blocks)


def body(tokens, up_weight, gate_weight, group_gain, mix_weight, mix_bias, out_gain, out_weight):
    own = tokens[0]

    def ring(shard, cut):
        shards, ahead, back = [shard], shard, shard
        for _ in range(1, HALF_CHIPS):
            ahead = lax.ppermute(ahead, "dp", along_z)
            back = lax.ppermute(back, "dp", against_z)
            shards += [ahead, back]
        shards.append(lax.ppermute(ahead[:cut], "dp", along_z))
        shards.append(lax.ppermute(back[cut:], "dp", against_z))
        return tuple(shards)

    left = lax.ppermute(own, "sp", along_x)
    right = lax.ppermute(own, "sp", against_x)
    packed_own = pl.pallas_call(
        pack_kernel,
        out_shape=jax.ShapeDtypeStruct((PACK, C), bf16),
        in_specs=[vmem, vmem],
        out_specs=vmem,
        compiler_params=params(56),
        name="pack_rows",
    )(gate_weight, up_weight)
    out_blocks = lax.all_gather(out_weight, "dp")

    weight_shards = ring(packed_own, PACK // 2)
    mix_shards = ring(mix_weight[0], 48)
    far_a = lax.ppermute(left[:HALF], "sp", along_x)
    far_b = lax.ppermute(right[HALF:], "sp", against_x)
    own_w = assemble(weight_shards)
    other_w = lax.ppermute(own_w, "dp", partner)
    own_rows = assemble(mix_shards)
    other_rows = lax.ppermute(own_rows, "dp", partner)
    rows = (own, left, right, far_a, far_b)

    nv = list(gate_rows((own_w, other_w), rows))
    for d, p in ((2, across_y), (1, along_y), (3, against_y)):
        nv[d] = lax.ppermute(nv[d], "sp", p)
    made = up_rows((own_w, other_w), rows)
    up = [made[0]]
    for n, p in ((2, along_x), (3, across_x), (1, against_x)):
        up.append(lax.ppermute(made[n], "sp", p))
    mixed = mix(own_rows, other_rows, group_gain, mix_bias, nv)
    mixed = lax.all_to_all(mixed, "sp", split_axis=0, concat_axis=0, tiled=True)
    opened = open_rows(up)
    return out_project(mixed, opened, out_gain.reshape(1, D), out_blocks)[None]


def solution(mesh):
    return jax.shard_map(
        body,
        mesh=mesh,
        in_specs=(
            P("dp", "sp", None),
            P("dp", None),
            P("dp", None),
            P("sp", None),
            P("sp", "dp", None),
            P("sp", None),
            P(),
            P(None, "dp"),
        ),
        out_specs=P("dp", "sp", None),
        check_vma=False,
    )
```

```python
import jax
import jax.numpy as jnp
from jax import lax
from jax.experimental import pallas as pl
from jax.experimental.pallas import tpu as pltpu
from jax.sharding import PartitionSpec as P


norm_eps = 1e-06
bf16 = jnp.bfloat16
f32 = jnp.float32

ROW = 4
DP = 16
C = 128
POS = 320
HALF = POS // 2
SPAN = 1280
D = 2048
K_DEV = D // DP
M_DEV = SPAN // DP
PROJ = ROW * K_DEV
PACK = 2 * PROJ
CHIPS = DP // 2
CUT = 48

along_x = [(y * 4 + x, y * 4 + (x + 1) % 4) for y in range(4) for x in range(4)]
against_x = [(b, a) for a, b in along_x]
across_x = [(y * 4 + x, y * 4 + (x + 2) % 4) for y in range(4) for x in range(4)]
along_y = [(y * 4 + x, (y + 1) % 4 * 4 + x) for y in range(4) for x in range(4)]
against_y = [(b, a) for a, b in along_y]
across_y = [(y * 4 + x, (y + 2) % 4 * 4 + x) for y in range(4) for x in range(4)]

along_z = [(2 * z + c, (2 * z + 2) % DP + c) for z in range(CHIPS) for c in range(2)]
against_z = [(b, a) for a, b in along_z]
partner = [(d, d ^ 1) for d in range(DP)]

vmem = pl.BlockSpec(memory_space=pltpu.VMEM)
hbm = pl.BlockSpec(memory_space=pltpu.HBM)


def params(mib):
    return pltpu.CompilerParams(vmem_limit_bytes=mib * 1024 * 1024)


def x_of():
    return lax.rem(lax.axis_index("sp"), ROW)


def y_of():
    return lax.div(lax.axis_index("sp"), ROW)


def pack_kernel(gate_ref, up_ref, out_ref, sems):
    x = x_of()
    copies = []
    for k in range(ROW):
        cols = pl.ds(pl.multiple_of((ROW * k + x) * C, C), C)
        for n, ref in enumerate((gate_ref, up_ref)):
            begin = n * PROJ + k * K_DEV
            target = out_ref.at[begin : begin + K_DEV, :]
            copies.append(pltpu.make_async_copy(ref.at[:, cols], target, sems.at[2 * k + n]))
    for copy in copies:
        copy.start()
    for copy in copies:
        copy.wait()


def assemble_kernel(*refs):
    shards, (far_a, far_b), out_ref = refs[:7], refs[7:9], refs[9]
    z = lax.div(lax.axis_index("dp"), 2)
    for ref, back in zip(shards, (0, 1, -1, 2, -2, 3, -3)):
        out_ref[lax.rem(z + CHIPS - back, CHIPS)] = ref[...]
    far = lax.rem(z + CHIPS // 2, CHIPS)
    out_ref[far, :CUT, :] = far_a[...]
    out_ref[far, CUT:, :] = far_b[...]


def assemble(shards):
    return pl.pallas_call(
        assemble_kernel,
        out_shape=jax.ShapeDtypeStruct((CHIPS, M_DEV, SPAN), bf16),
        in_specs=[vmem] * 9,
        out_specs=vmem,
        compiler_params=params(8),
        cost_estimate=pl.CostEstimate(flops=1_000_000, bytes_accessed=3_300_000, transcendentals=0),
        name="assemble_rows",
    )(*shards)


def gelu(v):
    return jax.nn.gelu(v, approximate=True)


def row_copies(pieces, rows_ref, sems):
    copies, begin = [], 0
    for n, ref in enumerate(pieces):
        copies.append(pltpu.make_async_copy(ref, rows_ref.at[begin : begin + ref.shape[0], :], sems.at[n]))
        begin += ref.shape[0]
    return copies


def gate_kernel(packed_ref, *refs):
    tokens, outs, (rows_ref, w_ref, row_sems, sems) = refs[:7], refs[7:11], refs[11:]
    y = y_of()
    x = x_of()
    copies = []
    for d in range(ROW):
        begin = pl.multiple_of(lax.rem(y + d, ROW) * K_DEV, K_DEV)
        copies.append(
            pltpu.make_async_copy(
                packed_ref.at[:, pl.ds(begin, K_DEV), :], w_ref.at[:, :, d * C : (d + 1) * C], sems.at[d]
            )
        )
    rows = row_copies(tokens, rows_ref, row_sems)
    for copy in copies + rows:
        copy.start()
    for copy in copies:
        copy.wait()
    weight = w_ref[...].reshape(D, ROW * C)
    for n, shift in enumerate((0, 3, 1, 2)):
        for copy in rows[:1] if n == 0 else rows[2 * n - 1 : 2 * n + 1]:
            copy.wait()
        made = jnp.dot(rows_ref[n * POS : (n + 1) * POS, :], weight, preferred_element_type=f32).astype(bf16)
        row = pl.multiple_of(lax.rem(x + shift, ROW) * POS, POS)
        act = gelu(made.astype(f32))
        for d in range(ROW):
            part = act[:, d * C : (d + 1) * C]
            center = jnp.mean(part, axis=-1, keepdims=True)
            part = part - center
            spread = jnp.mean(part * part, axis=-1, keepdims=True)
            outs[d][pl.ds(row, POS), :] = (part * lax.rsqrt(spread + norm_eps)).astype(bf16)


row_scratch = [
    pltpu.VMEM((SPAN, D), bf16),
    pltpu.VMEM((DP, K_DEV, ROW * C), bf16),
    pltpu.SemaphoreType.DMA((7,)),
    pltpu.SemaphoreType.DMA((ROW,)),
]


def gate_rows(packed, tokens):
    return pl.pallas_call(
        gate_kernel,
        out_shape=[jax.ShapeDtypeStruct((SPAN, C), bf16)] * ROW,
        in_specs=[hbm] * 8,
        out_specs=[vmem] * ROW,
        scratch_shapes=row_scratch,
        compiler_params=params(52),
        cost_estimate=pl.CostEstimate(
            flops=2 * SPAN * D * ROW * C, bytes_accessed=10_000_000, transcendentals=SPAN * ROW * C
        ),
        name="gate_rows",
    )(packed, *tokens)


def up_kernel(packed_ref, *refs):
    tokens, outs, (rows_ref, w_ref, row_sems, sems) = refs[:7], refs[7:11], refs[11:]
    copies = []
    for k in range(ROW):
        copies.append(
            pltpu.make_async_copy(
                packed_ref.at[:, PROJ + k * K_DEV : PROJ + (k + 1) * K_DEV, :],
                w_ref.at[:, :, k * C : (k + 1) * C],
                sems.at[k],
            )
        )
    rows = row_copies(tokens, rows_ref, row_sems)
    for copy in copies + rows:
        copy.start()
    for copy in copies:
        copy.wait()
    weight = w_ref[...].reshape(D, ROW * C)
    for n in range(ROW):
        for copy in rows[:1] if n == 0 else rows[2 * n - 1 : 2 * n + 1]:
            copy.wait()
        made = jnp.dot(rows_ref[n * POS : (n + 1) * POS, :], weight, preferred_element_type=f32)
        outs[n][...] = made.astype(bf16)


def up_rows(packed, tokens):
    return pl.pallas_call(
        up_kernel,
        out_shape=[jax.ShapeDtypeStruct((POS, ROW * C), bf16)] * ROW,
        in_specs=[hbm] * 8,
        out_specs=[vmem] * ROW,
        scratch_shapes=row_scratch,
        compiler_params=params(52),
        cost_estimate=pl.CostEstimate(flops=2 * SPAN * D * ROW * C, bytes_accessed=10_000_000, transcendentals=0),
        name="up_rows",
    )(packed, *tokens)


def mix_kernel(own_ref, other_ref, gain_ref, bias_ref, *refs):
    nv, (out_ref, bias_cols) = refs[:ROW], refs[ROW:]
    core = lax.rem(lax.axis_index("dp"), 2)
    y = y_of()
    gain = gain_ref[...]
    bias_cols[...] = jnp.broadcast_to(bias_ref[...], (C, SPAN)).T
    values = jnp.concatenate([ref[...] for ref in nv], axis=1)
    for t in range(ROW):
        width = -(-(t + 1) * POS // C) * C
        begin = t * POS
        parts = ((own_ref, 2 * t, core), (own_ref, 2 * t + 1, core + 2))
        parts += ((other_ref, 2 * t, 1 - core), (other_ref, 2 * t + 1, 3 - core))
        masked = []
        for ref, shard, row in parts:
            rows = ref[shard, :, :width]
            i = lax.broadcasted_iota(jnp.int32, (M_DEV, width), 0) + (begin + row * M_DEV)
            j = lax.broadcasted_iota(jnp.int32, (M_DEV, width), 1)
            masked.append(jnp.where(j <= i, rows, jnp.zeros_like(rows)))
        made = jnp.dot(jnp.concatenate(masked, axis=0), values[:width, :], preferred_element_type=f32)
        for d in range(ROW):
            block = lax.rem(y + ROW - d, ROW)
            for n, (_, _, row) in enumerate(parts):
                at = pl.multiple_of(row * M_DEV, 16)
                part = made[n * M_DEV : (n + 1) * M_DEV, d * C : (d + 1) * C] * gain
                part = part + bias_cols[pl.ds(begin + at, M_DEV), :]
                out_ref[block * ROW + t, pl.ds(at, M_DEV), :] = part.astype(bf16)


def mix(own, other, gain, bias, nv):
    return pl.pallas_call(
        mix_kernel,
        out_shape=jax.ShapeDtypeStruct((ROW * ROW, POS, C), bf16),
        in_specs=[vmem] * 8,
        out_specs=vmem,
        scratch_shapes=[pltpu.VMEM((SPAN, C), f32)],
        compiler_params=params(16),
        cost_estimate=pl.CostEstimate(flops=2 * SPAN * SPAN * ROW * C, bytes_accessed=7_000_000, transcendentals=0),
        name="mix_positions",
    )(own, other, gain, bias, *nv)


def open_kernel(*refs):
    up, out_ref = refs[:ROW], refs[ROW]
    x = x_of()
    for e in range(ROW):
        source = lax.rem(x + ROW - e, ROW)
        for k in range(ROW):
            out_ref[k * ROW + source] = gelu(up[e][:, k * C : (k + 1) * C].astype(f32))


def open_rows(up):
    return pl.pallas_call(
        open_kernel,
        out_shape=jax.ShapeDtypeStruct((ROW * ROW, POS, C), f32),
        in_specs=[vmem] * ROW,
        out_specs=vmem,
        compiler_params=params(12),
        cost_estimate=pl.CostEstimate(flops=POS * D * 10, bytes_accessed=4_000_000, transcendentals=POS * D),
        name="open_rows",
    )(*up)


def out_kernel(mixed_ref, opened_ref, gain_ref, blocks_ref, out_ref, gated_ref, w_ref, made_ref, sems, out_sems):
    steps = DP // 4
    copies = [
        pltpu.make_async_copy(blocks_ref.at[4 * n : 4 * n + 4], w_ref.at[4 * n : 4 * n + 4], sems.at[n])
        for n in range(steps)
    ]
    for copy in copies:
        copy.start()
    total = jnp.zeros((POS, C), f32)
    for g in range(ROW * ROW):
        cols = slice(g * C, (g + 1) * C)
        gated = (opened_ref[g] * mixed_ref[g].astype(f32)).astype(bf16).astype(f32)
        gated_ref[:, cols] = (gated * gain_ref[:, cols]).astype(bf16)
        total = total + gated * gated
    scale = lax.rsqrt(jnp.sum(total, axis=-1, keepdims=True) / D + norm_eps)
    writes = []
    for n in range(steps):
        copies[n].wait()
        weight = jnp.concatenate([w_ref[4 * n + k] for k in range(4)], axis=1)
        made = jnp.dot(gated_ref[...], weight, preferred_element_type=f32)
        cols = slice(4 * n * K_DEV, 4 * (n + 1) * K_DEV)
        made_ref[:, cols] = (made * scale).astype(bf16)
        writes.append(pltpu.make_async_copy(made_ref.at[:, cols], out_ref.at[:, cols], out_sems.at[n]))
        writes[n].start()
    for write in writes:
        write.wait()


def out_project(mixed, opened, gain, blocks):
    return pl.pallas_call(
        out_kernel,
        out_shape=jax.ShapeDtypeStruct((POS, D), bf16),
        in_specs=[vmem, vmem, vmem, hbm],
        out_specs=hbm,
        scratch_shapes=[
            pltpu.VMEM((POS, D), bf16),
            pltpu.VMEM((DP, D, K_DEV), bf16),
            pltpu.VMEM((POS, D), bf16),
            pltpu.SemaphoreType.DMA((DP // 4,)),
            pltpu.SemaphoreType.DMA((DP // 4,)),
        ],
        compiler_params=params(45),
        cost_estimate=pl.CostEstimate(flops=2 * POS * D * D, bytes_accessed=13_000_000, transcendentals=0),
        name="norm_out",
    )(mixed, opened, gain, blocks)


def body(tokens, up_weight, gate_weight, group_gain, mix_weight, mix_bias, out_gain, out_weight):
    own = tokens[0]
    shard = mix_weight[0]

    packed_own = pl.pallas_call(
        pack_kernel,
        out_shape=jax.ShapeDtypeStruct((PACK, C), bf16),
        in_specs=[hbm, hbm],
        out_specs=vmem,
        scratch_shapes=[pltpu.SemaphoreType.DMA((2 * ROW,))],
        compiler_params=params(56),
        name="pack_rows",
    )(gate_weight, up_weight)
    packed = lax.all_gather(packed_own, "dp")
    out_shard, _ = lax.optimization_barrier((out_weight, packed_own))
    out_blocks = lax.all_gather(out_shard, "dp")

    head, tail = own[:HALF], own[HALF:]
    left_a = lax.ppermute(head, "sp", along_x)
    right_b = lax.ppermute(tail, "sp", against_x)
    left_b = lax.ppermute(tail, "sp", along_x)
    right_a = lax.ppermute(head, "sp", against_x)
    one_p = lax.ppermute(shard, "dp", along_z)
    one_m = lax.ppermute(shard, "dp", against_z)
    two_p = lax.ppermute(one_p, "dp", along_z)
    two_m = lax.ppermute(one_m, "dp", against_z)
    far_a = lax.ppermute(left_a, "sp", along_x)
    far_b = lax.ppermute(right_b, "sp", against_x)
    three_p = lax.ppermute(two_p, "dp", along_z)
    three_m = lax.ppermute(two_m, "dp", against_z)
    four_p = lax.ppermute(three_p[:CUT], "dp", along_z)
    four_m = lax.ppermute(three_m[CUT:], "dp", against_z)
    own_rows = assemble((shard, one_p, one_m, two_p, two_m, three_p, three_m, four_p, four_m))
    other_rows = lax.ppermute(own_rows, "dp", partner)
    rows = (own, left_a, left_b, right_a, right_b, far_a, far_b)

    nv = list(gate_rows(packed, rows))
    for d, p in ((2, across_y), (1, along_y), (3, against_y)):
        nv[d] = lax.ppermute(nv[d], "sp", p)
    made = up_rows(packed, rows)
    up = [made[0]]
    for n, p in ((2, along_x), (3, across_x), (1, against_x)):
        up.append(lax.ppermute(made[n], "sp", p))
    mixed = mix(own_rows, other_rows, group_gain, mix_bias, nv)
    mixed = lax.all_to_all(mixed, "sp", split_axis=0, concat_axis=0, tiled=True)
    opened = open_rows(up)
    return out_project(mixed, opened, out_gain.reshape(1, D), out_blocks)[None]


def solution(mesh):
    return jax.shard_map(
        body,
        mesh=mesh,
        in_specs=(
            P("dp", "sp", None),
            P("dp", None),
            P("dp", None),
            P("sp", None),
            P("sp", "dp", None),
            P("sp", None),
            P(),
            P(None, "dp"),
        ),
        out_specs=P("dp", "sp", None),
        check_vma=False,
    )
```
